128 devices in a mesh: grp: 4 (over y, x), ep: 32 (over z, core).
Axes of the slice: x: 2, y: 2, z: 16, core: 2. Of those that a mesh axis runs over, the one named last changes fastest.
The devices are a block of a 8x8x16 slice.
Arguments:
- tokens: bfloat16 [4096, 2048], P(('grp', 'ep')), parts along dimension 0, may hold values from -6 to 6
- routes: int32 [4096, 4], P(('grp', 'ep')), parts along dimension 0, may hold values from 0 to 31, all different within a row; in each aligned block of 32 rows (0 to 31, 32 to 63, ...) at most 8 rows name the same one
- route_logits: float32 [4096, 4], P(('grp', 'ep')), parts along dimension 0, may hold values from -4 to 4
- state_real: float32 [4096, 64, 64], P('grp', 'ep'), parts along dimension 0, may hold values from -4 to 4
- state_imag: float32 [4096, 64, 64], P('grp', 'ep'), parts along dimension 0, may hold values from -4 to 4
- gain_in: float32 [2048], replicated, may hold values from 0.1 to 1.9
- proj_in: bfloat16 [2048, 1024], P(None, 'ep'), may hold values from -0.125 to 0.125
- decay_rate: float32 [64, 64], P('ep'), may hold values from 0.05 to 2
- frequency: float32 [64, 64], P('ep'), may hold values from -4 to 4
- log_step: float32 [64], P('ep'), may hold values from -3 to 0
- input_real: float32 [64, 64, 16], P('ep'), may hold values from -1 to 1
- input_imag: float32 [64, 64, 16], P('ep'), may hold values from -1 to 1
- output_real: float32 [64, 16, 64], P('ep'), may hold values from -0.5 to 0.5
- output_imag: float32 [64, 16, 64], P('ep'), may hold values from -0.5 to 0.5
- skip_gain: float32 [64, 16], P('ep'), may hold values from -4 to 4
- proj_out: bfloat16 [1024, 2048], P('ep'), may hold values from -0.1875 to 0.1875
- gain_mid: float32 [2048], replicated, may hold values from 0.1 to 1.9
- expert_gate: bfloat16 [32, 2048, 1024], P('ep'), may hold values from -0.33007812 to 0.33007812
- expert_up: bfloat16 [32, 2048, 1024], P('ep'), may hold values from -0.33007812 to 0.33007812
- expert_down: bfloat16 [32, 1024, 2048], P('ep'), may hold values from -0.056152344 to 0.056152344
- dense_gate: bfloat16 [2048, 2048], P(None, 'ep'), may hold values from -0.125 to 0.125
- dense_up: bfloat16 [2048, 2048], P(None, 'ep'), may hold values from -0.125 to 0.125
- dense_down: bfloat16 [2048, 2048], P('ep'), may hold values from -0.125 to 0.125
- dense_mix: float32 [2048], P('ep'), may hold values from -0.39774758 to 0.39774758
Outputs:
- layer_out: bfloat16 [4096, 2048], P(('grp', 'ep')), parts along dimension 0
- state_real_new: float32 [4096, 64, 64], P('grp', 'ep'), parts along dimension 0
- state_imag_new: float32 [4096, 64, 64], P('grp', 'ep'), parts along dimension 0
The draws below stay inside these ranges and needn't reach their ends.
There are 4 independent parts, one for each index of `grp`. The reference program is written for one: setup_inputs(seed, part) draws one part's arguments, and reference() takes and returns one part's arrays. A program takes and returns all parts, laid end to end along the dimension named above; an argument that names none is the same for every part. Nothing has to cross between parts.
Inputs may be any that keep to these rules, and one draw needn't show every extreme that they name: `routes`: each row names 4 different experts; among the rows of one device no expert is named more than 8 times, and in every draw some device names some expert exactly 8 times.
All inputs are finite; a program needn't handle non-finite values.
Results may differ from the reference program's by a relative error of at most 0.015.
Values may be sent and summed in bfloat16 or wider, within the bound.
A program may use at most 128 MiB of HBM per device.

```python
import math
import jax
import jax.numpy as jnp
import numpy as np
from jax import lax

D = 2048
CHANNELS = 1024
GROUP = 16
GROUPS = 64
STATE = 64
FF = 1024
DENSE = 2048
TOPK = 4
EXPERTS = 32
SEQ_DEV = 32
SEQS = 1024
CAP = 8
N_EP = 32


def block_scale(key, shape, split, smallest, top_value):
    def one(axis_at, parts):
        steps = jax.random.uniform(jax.random.fold_in(jax.random.fold_in(key, 6), axis_at), (parts,), jnp.float32, smallest / len(split), top_value / len(split))
        return jnp.repeat(jnp.exp(steps), shape[axis_at] // parts).reshape((-1,) + (1,) * (len(shape) - axis_at - 1))

    gain = one(*split[0])
    for cut in split[1:]:
        gain = gain * one(*cut)
    return gain


def assign_block(key, own, number, rows, count, top, most, slope):
    sequence = jax.random.permutation(key, count)
    heavy_load, ordinary = load_shares(count, rows * top, most, slope, True), load_shares(count, rows * top, most, slope, False)
    places = jnp.arange(count)

    def named(lengths, rotation):
        used = int((lengths > 0).sum())
        fixed = max(1, used // 4)
        moved = fixed + (places - fixed + rotation * (used - fixed)) % max(1, count - fixed)
        return jnp.zeros((count,), jnp.int32).at[sequence[jnp.where(places < fixed, places, moved)]].set(jnp.asarray(lengths, jnp.int32))

    lengths = jnp.where(number % 4 == 0, named(heavy_load, number // 4), named(ordinary, number - number // 4 - 1))
    mixed = jax.random.permutation(jax.random.fold_in(own, 3), count)
    source_of, taker = mixed[0:count // 2 * 2:2], mixed[1:count // 2 * 2:2]
    slack = jnp.minimum(lengths[source_of] - 1, most - lengths[taker]) // 2
    slack = jnp.where((source_of == sequence[0]) | (taker == sequence[0]) | (lengths[taker] == 0), 0, jnp.maximum(slack, 0))
    moved = jax.random.randint(jax.random.fold_in(own, 4), (count // 2,), 0, 1 << 20) % (slack + 1)
    lengths = lengths.at[source_of].add(-moved).at[taker].add(moved)
    labels = jnp.searchsorted(jnp.cumsum(lengths), jnp.arange(rows * top), side="right").astype(jnp.int32)
    table = labels.reshape(top, rows).T
    table = table[jax.random.permutation(jax.random.fold_in(own, 1), rows)]
    rotation = jax.random.randint(jax.random.fold_in(own, 2), (rows, 1), 0, top)
    return jnp.take_along_axis(table, (jnp.arange(top)[None, :] + rotation) % top, axis=1)


def load_shares(amount, total, limit, skew, full):
    loads = [(1 << 20) // math.isqrt(grade ** skew) + 1 for grade in range(1, amount + 1)]
    largest = limit if full else min(limit, max(-(-total // amount), total * loads[0] // sum(loads)))
    least = 1 if total - largest >= amount - 1 else 0
    given, rest = [largest] + [least] * (amount - 1), total - largest - least * (amount - 1)
    while rest > 0:
        candidates = [i for i in range(1, amount) if given[i] < largest] or [i for i in range(1, amount) if given[i] < limit]
        mass, remaining = sum([loads[i] for i in candidates]), rest
        for i in candidates:
            addition = min(limit - given[i], max(1, remaining * loads[i] // mass), rest)
            given[i] = given[i] + addition
            rest = rest - addition
    return np.array(given)


def gaussian(own_key, extent, spread, most, shards=(), kind=jnp.bfloat16):
    loudness = block_scale(own_key, extent, shards, -0.22, 0.18) if shards else 1.0
    entries = jax.random.normal(own_key, extent, jnp.float32) * spread * loudness
    return jnp.minimum(jnp.maximum(entries, -most), most).astype(kind)


def setup_inputs(seed: int = 0, part: int = 0) -> dict:
    splits = jax.random.split(jax.random.key(seed), 25)
    part_keys = jax.random.split(jax.random.fold_in(splits[24], part), 25)
    tokens = gaussian(part_keys[0], (SEQS, D), 1.0, 6.0, ((0, 32),))
    routes_keys = jax.random.split(jax.random.fold_in(part_keys[1], 1), SEQS // SEQ_DEV)
    routes_turns = jax.random.permutation(jax.random.fold_in(part_keys[1], 3), SEQS // SEQ_DEV)
    routes = jax.vmap(lambda own, number: assign_block(jax.random.fold_in(part_keys[1], 2), own, number, SEQ_DEV, EXPERTS, TOPK, CAP, 2))(routes_keys, routes_turns).reshape((SEQS, TOPK))
    route_logits = gaussian(part_keys[2], (SEQS, TOPK), 1.0, 4.0, ((0, 32),), jnp.float32)
    state_real = gaussian(part_keys[3], (SEQS, GROUPS, STATE), 0.5, 4.0, ((1, 32),), jnp.float32)
    state_imag = gaussian(part_keys[4], (SEQS, GROUPS, STATE), 0.5, 4.0, ((1, 32),), jnp.float32)
    gain_in = jnp.clip(1.0 + 0.18 * jax.random.normal(splits[5], (D,), jnp.float32), 0.1, 1.9)
    proj_in = gaussian(splits[6], (D, CHANNELS), D ** -0.5, 0.125, ((1, 32),))
    decay_rate = jnp.clip(jnp.exp(math.log(2.0) - 3.6888794 * jax.random.uniform(splits[7], (GROUPS, STATE), jnp.float32) ** block_scale(splits[7], (GROUPS, STATE), ((0, 32),), -0.2, 0.2)), 0.05, 2.0)
    frequency = jnp.clip(jax.random.uniform(splits[8], (GROUPS, STATE), jnp.float32, -4.0, 4.0) * block_scale(splits[8], (GROUPS, STATE), ((0, 32),), -0.4, 0.0), -4.0, 4.0)
    log_step = jnp.clip(-3.0 + 3.0 * jax.random.uniform(splits[9], (GROUPS,), jnp.float32) ** block_scale(splits[9], (GROUPS,), ((0, 32),), -0.2, 0.2), -3.0, 0.0)
    input_real = gaussian(splits[10], (GROUPS, STATE, GROUP), (2 * GROUP) ** -0.5, 1.0, ((0, 32),), jnp.float32)
    input_imag = gaussian(splits[11], (GROUPS, STATE, GROUP), (2 * GROUP) ** -0.5, 1.0, ((0, 32),), jnp.float32)
    output_real = gaussian(splits[12], (GROUPS, GROUP, STATE), (2 * STATE) ** -0.5, 0.5, ((0, 32),), jnp.float32)
    output_imag = gaussian(splits[13], (GROUPS, GROUP, STATE), (2 * STATE) ** -0.5, 0.5, ((0, 32),), jnp.float32)
    skip_gain = gaussian(splits[14], (GROUPS, GROUP), 1.0, 4.0, ((0, 32),), jnp.float32)
    proj_out = gaussian(splits[15], (CHANNELS, D), CHANNELS ** -0.5, 0.1875, ((0, 32),))
    gain_mid = jnp.clip(1.0 + 0.18 * jax.random.normal(splits[16], (D,), jnp.float32), 0.1, 1.9)
    expert_gate = gaussian(splits[17], (EXPERTS, D, FF), (2.5 / D ** 0.5), 0.33007812, ((0, 32),))
    expert_up = gaussian(splits[18], (EXPERTS, D, FF), (2.5 / D ** 0.5), 0.33007812, ((0, 32),))
    expert_down = gaussian(splits[19], (EXPERTS, FF, D), (0.3 / FF ** 0.5), 0.056152344, ((0, 32),))
    dense_gate = gaussian(splits[20], (D, DENSE), D ** -0.5, 0.125, ((1, 32),))
    dense_up = gaussian(splits[21], (D, DENSE), D ** -0.5, 0.125, ((1, 32),))
    dense_down = gaussian(splits[22], (DENSE, D), DENSE ** -0.5, 0.125, ((0, 32),))
    dense_mix = gaussian(splits[23], (DENSE,), (3.0 / DENSE ** 0.5), 0.39774758, ((0, 32),), jnp.float32)
    return {"tokens": tokens, "routes": routes, "route_logits": route_logits, "state_real": state_real, "state_imag": state_imag, "gain_in": gain_in, "proj_in": proj_in, "decay_rate": decay_rate, "frequency": frequency, "log_step": log_step, "input_real": input_real, "input_imag": input_imag, "output_real": output_real, "output_imag": output_imag, "skip_gain": skip_gain, "proj_out": proj_out, "gain_mid": gain_mid, "expert_gate": expert_gate, "expert_up": expert_up, "expert_down": expert_down, "dense_gate": dense_gate, "dense_up": dense_up, "dense_down": dense_down, "dense_mix": dense_mix}


EPS = 1e-06
LIMIT = 7.0
ALPHA = 1.702
HIGH = lax.Precision.HIGHEST

def rms_scale(values, gain_vec):
    return values * lax.rsqrt(lax.optimization_barrier(jnp.mean(values * values, axis=-1, keepdims=True)) + EPS) * gain_vec

def state_step(unit_rows, state_real, state_imag, decay_rate, frequency, log_step, input_real, input_imag, output_real, output_imag, skip_gain):
    seq_count = unit_rows.shape[0]
    groups, group_size = skip_gain.shape
    inputs = unit_rows.astype(jnp.float32).reshape(seq_count, groups, group_size)
    step_size = jnp.exp(log_step)[:, None]
    decay_part = -decay_rate
    magnitude = jnp.exp(decay_part * step_size)
    carry_real = magnitude * jnp.cos(frequency * step_size)
    carry_imag = magnitude * jnp.sin(frequency * step_size)
    denom = decay_part * decay_part + frequency * frequency
    feed_real = ((carry_real - 1.0) * decay_part + carry_imag * frequency) / denom
    feed_imag = (carry_imag * decay_part - (carry_real - 1.0) * frequency) / denom
    drive_real = jnp.einsum('sgp,gnp->sgn', inputs, input_real, precision=HIGH)
    drive_imag = jnp.einsum('sgp,gnp->sgn', inputs, input_imag, precision=HIGH)
    new_real = carry_real * state_real - carry_imag * state_imag + feed_real * drive_real - feed_imag * drive_imag
    new_imag = carry_real * state_imag + carry_imag * state_real + feed_real * drive_imag + feed_imag * drive_real
    readout = jnp.einsum('gpn,sgn->sgp', output_real, new_real, precision=HIGH) - jnp.einsum('gpn,sgn->sgp', output_imag, new_imag, precision=HIGH) + skip_gain * inputs
    branch = jax.nn.gelu(readout).reshape(seq_count, groups * group_size).astype(jnp.bfloat16)
    return (branch, new_real, new_imag)

def expert_apply(row_block, gate_weight, up_weight, down_weight):
    gated = jnp.minimum(jnp.dot(row_block, gate_weight, preferred_element_type=jnp.float32), LIMIT)
    upper = jnp.clip(jnp.dot(row_block, up_weight, preferred_element_type=jnp.float32), -LIMIT, LIMIT)
    activated = ((upper + 1.0) * gated * jax.nn.sigmoid(ALPHA * gated)).astype(jnp.bfloat16)
    return jnp.dot(activated, down_weight, preferred_element_type=jnp.float32).astype(jnp.bfloat16)

def reference(tokens, routes, route_logits, state_real, state_imag, gain_in, proj_in, decay_rate, frequency, log_step, input_real, input_imag, output_real, output_imag, skip_gain, proj_out, gain_mid, expert_gate, expert_up, expert_down, dense_gate, dense_up, dense_down, dense_mix):
    inputs = tokens.astype(jnp.float32)
    normed = rms_scale(inputs, gain_in).astype(jnp.bfloat16)
    unit_rows = jnp.dot(normed, proj_in, preferred_element_type=jnp.float32).astype(jnp.bfloat16)
    branch, new_real, new_imag = state_step(unit_rows, state_real, state_imag, decay_rate, frequency, log_step, input_real, input_imag, output_real, output_imag, skip_gain)
    residual = inputs + jnp.dot(branch, proj_out, preferred_element_type=jnp.float32)
    mixed = rms_scale(residual, gain_mid).astype(jnp.bfloat16)
    weights = jnp.exp(route_logits)
    weights = weights / lax.optimization_barrier(jnp.sum(weights, axis=1, keepdims=True))
    limit_rows = N_EP * CAP
    expert_count = expert_gate.shape[0]

    def one_expert(running, expert_index):
        shares = lax.optimization_barrier(jnp.sum(jnp.where(routes == expert_index, weights, 0.0), axis=1))
        marked = jnp.any(routes == expert_index, axis=1).astype(jnp.int32)
        order_rows = jnp.argsort(1 - marked, stable=True)[:limit_rows].astype(jnp.int32)
        picked = jnp.take(mixed, order_rows, axis=0)
        result = expert_apply(picked, expert_gate[expert_index], expert_up[expert_index], expert_down[expert_index])
        running = running.at[order_rows].add(shares[order_rows][:, None] * result.astype(jnp.float32))
        return (running, None)
    routed, _ = lax.scan(one_expert, jnp.zeros(residual.shape, jnp.float32), jnp.arange(expert_count, dtype=jnp.int32))
    hidden = (jax.nn.silu(jnp.dot(mixed, dense_gate, preferred_element_type=jnp.float32)) * jnp.dot(mixed, dense_up, preferred_element_type=jnp.float32)).astype(jnp.bfloat16)
    dense_out = jnp.dot(hidden, dense_down, preferred_element_type=jnp.float32)
    gate_logit = jnp.dot(hidden.astype(jnp.float32), dense_mix, precision=HIGH)
    layer_out = (residual + routed + jax.nn.sigmoid(gate_logit)[:, None] * dense_out).astype(jnp.bfloat16)
    return (layer_out, new_real, new_imag)
```

```python
import functools

import jax
import jax.numpy as jnp
from jax import lax
from jax.experimental import pallas as pl
from jax.experimental.pallas import tpu as pltpu
from jax.sharding import PartitionSpec as P

EPS = 1e-06
LIMIT = 7.0
ALPHA = 1.702
MESH = pl.DeviceIdType.MESH
F32 = jnp.float32
BF16 = jnp.bfloat16
NT = (((1,), (1,)), ((), ()))


def dot(a, b):
    return jnp.dot(a, b, preferred_element_type=F32)


def dot_nt(a, b):
    return lax.dot_general(a, b, NT, preferred_element_type=F32)


def iota(shape, dim):
    return lax.broadcasted_iota(jnp.int32, shape, dim)


class Ring:
    def __init__(self, pieces, send, recv, where):
        self.pieces, self.send, self.recv, self.where = pieces, send, recv, where
        self.count = len(pieces)

    def copy(self, step, way, q):
        ref = self.pieces[q](self.where["block"](step, way))
        return pltpu.make_async_remote_copy(
            src_ref=ref,
            dst_ref=ref,
            send_sem=self.send.at[way, q],
            recv_sem=self.recv.at[way, step, q],
            device_id={"ep": self.where["next"][way]},
            device_id_type=MESH,
        )

    def arrival(self, step, way, q):
        ref = self.pieces[q](self.where["block"](step + 1, way))
        return pltpu.make_async_remote_copy(
            src_ref=ref,
            dst_ref=ref,
            send_sem=self.send.at[way, q],
            recv_sem=self.recv.at[way, step, q],
            device_id={"ep": self.where["next"][way]},
            device_id_type=MESH,
        )

    def half(self, way):
        mid = self.count // 2
        return range(mid) if way == 0 else range(mid, self.count)

    def first(self):
        for q in range(self.count):
            for way in (0, 1):
                self.copy(0, way, q).start()

    def piece(self, step, way, q, last=False):
        self.arrival(step - 1, way, q).wait_recv()
        self.copy(step - 1, way, q).wait_send()
        if not last or q in self.half(way):
            self.copy(step, way, q).start()

    def finish(self, hops):
        for way in (0, 1):
            for q in self.half(way):
                self.arrival(hops - 1, way, q).wait_recv()
                self.copy(hops - 1, way, q).wait_send()


def kernel(
    n,
    dims,
    tokens,
    routes_t,
    logits_t,
    state_re,
    state_im,
    gain_in,
    proj_in_t,
    params,
    in_re,
    in_im,
    out_re,
    out_im,
    proj_out,
    gain_mid,
    expert_gate,
    expert_up,
    expert_down,
    dense_gate_t,
    dense_up_t,
    dense_down,
    layer_out,
    new_re,
    new_im,
    rows_all,
    proj_all,
    branch_all,
    lhs_all,
    resid,
    own_res,
    mixed,
    w_gate,
    w_up,
    w_down,
    s_re,
    s_im,
    o_re,
    o_im,
    picked,
    active,
    down_rhs,
    combined,
    partner_part,
    ring_in,
    ring_out,
    units,
    pin4,
    dense_gu,
    hidden,
    logit_all,
    square,
    local_sem,
    out_sem,
    t_send,
    t_recv,
    p1_send,
    p1_recv,
    p2_send,
    p2_recv,
    b_send,
    b_recv,
    r_send,
    r_recv,
    td_send,
    td_recv,
    p1d_send,
    p1d_recv,
    p2d_send,
    p2d_recv,
    bd_send,
    bd_recv,
    cd_send,
    cd_recv,
    l_send,
    l_recv,
):
    rows, width, ff, cap = dims
    chips = n // 2
    hops = chips // 2
    seqs = n * rows
    block = seqs // 4
    per_block = n // 4
    slots = per_block * cap
    me = lax.axis_index("ep")
    chip = me // 2
    core = me % 2
    other = 1 - core
    partner = chip * 2 + other
    right = ((chip + 1) % chips) * 2 + core
    left = ((chip + chips - 1) % chips) * 2 + core
    nexts = (right, left)

    def block_of(step, way):
        at = (chip - step + chips) % chips if way == 0 else (chip + step) % chips
        return at * 2 + core

    where = {"next": nexts, "block": block_of}

    half_rows = rows // 2
    local = [
        pltpu.make_async_copy(tokens, rows_all.at[me, :, pl.ds(0, width)], local_sem.at[0]),
        pltpu.make_async_copy(proj_out, proj_all.at[me], local_sem.at[1]),
        pltpu.make_async_copy(state_re, s_re, local_sem.at[2]),
        pltpu.make_async_copy(state_im, s_im, local_sem.at[3]),
        pltpu.make_async_copy(expert_gate, w_gate, local_sem.at[4]),
        pltpu.make_async_copy(expert_up, w_up, local_sem.at[5]),
        pltpu.make_async_copy(expert_down, w_down, local_sem.at[6]),
    ]
    for i in range(4):
        local.append(pltpu.make_async_copy(proj_in_t, pin4.at[pl.ds(32 * i, 32)], local_sem.at[7 + i]))
        local.append(pltpu.make_async_copy(dense_down, down_rhs.at[i, pl.ds(0, 64)], local_sem.at[11 + i]))
    local.append(pltpu.make_async_copy(dense_gate_t, dense_gu.at[pl.ds(0, 64)], local_sem.at[15]))
    local.append(pltpu.make_async_copy(dense_up_t, dense_gu.at[pl.ds(64, 64)], local_sem.at[16]))
    for c in local:
        c.start()

    barrier = pltpu.get_barrier_semaphore()
    for peer in (left, right, partner):
        pl.semaphore_signal(barrier, inc=1, device_id={"ep": peer}, device_id_type=MESH)

    expert_row = iota((128, rows), 0)
    expert_id = expert_row % n
    scores = jnp.exp(logits_t[...])
    scores = scores / jnp.sum(scores, axis=0, keepdims=True)
    top = scores.shape[0]
    share = jnp.zeros((128, rows), F32)
    for k in range(top):
        share = share + jnp.where(routes_t[k : k + 1, :] == expert_id, scores[k : k + 1, :], 0.0)
    mark = jnp.where(share > 0.0, 1.0, 0.0)
    upper = jnp.where(iota((rows, rows), 0) <= iota((rows, rows), 1), 1.0, 0.0)
    rank = dot(mark.astype(BF16), upper.astype(BF16)) * mark
    part_hi = share.astype(BF16).astype(F32)
    kind = expert_row // n
    extra = jnp.where(
        kind == 0, part_hi, jnp.where(kind == 1, share - part_hi, jnp.where(kind == 2, rank, 0.0))
    )
    square[...] = jnp.zeros(square.shape, F32)
    square[:, 0:rows] = extra
    rows_all[me, :, width : width + 128] = square[...].T[0:rows, :].astype(BF16)

    pl.semaphore_wait(barrier, 3)

    ext = width + 128
    cut = ((ext // 128 + 1) // 2) * 128
    half_w = width // 2

    def row_piece(r0, c0, c1):
        return lambda dev: rows_all.at[dev, pl.ds(r0, half_rows), pl.ds(c0, c1 - c0)]

    def proj_piece(r0, c0):
        return lambda dev: proj_all.at[dev, pl.ds(r0, half_rows), pl.ds(c0, half_w)]

    def branch_piece(r0):
        return lambda dev: branch_all.at[dev, pl.ds(r0, block // 2)]

    t_ring = Ring(
        [
            row_piece(0, 0, cut),
            row_piece(0, cut, ext),
            row_piece(half_rows, 0, cut),
            row_piece(half_rows, cut, ext),
        ],
        t_send,
        t_recv,
        where,
    )
    p1_ring = Ring([proj_piece(0, 0), proj_piece(0, half_w)], p1_send, p1_recv, where)
    p2_ring = Ring([proj_piece(half_rows, 0), proj_piece(half_rows, half_w)], p2_send, p2_recv, where)
    b_ring = Ring([branch_piece(0), branch_piece(block // 2)], b_send, b_recv, where)

    class Share:
        def __init__(self, ref, send, recv):
            self.ref, self.send, self.recv = ref, send, recv

        def copy(self, dist, way, which):
            ref = self.ref(block_of(dist, way) // 2 * 2 + which)
            return pltpu.make_async_remote_copy(
                src_ref=ref,
                dst_ref=ref,
                send_sem=self.send.at[way],
                recv_sem=self.recv.at[way, dist],
                device_id={"ep": partner},
                device_id_type=MESH,
            )

        def give(self, dist, way, used=True):
            if used:
                self.copy(dist, way, core).wait_send()
            self.copy(dist, way, core).start()

        def take(self, dist, way):
            self.copy(dist, way, other).wait_recv()

        def close(self, dist):
            for way in (0, 1):
                self.copy(dist, way, core).wait_send()

    t_share = Share(lambda dev: rows_all.at[dev], td_send, td_recv)
    p1_share = Share(lambda dev: proj_all.at[dev, pl.ds(0, half_rows)], p1d_send, p1d_recv)
    p2_share = Share(lambda dev: proj_all.at[dev, pl.ds(half_rows, half_rows)], p2d_send, p2d_recv)
    b_share = Share(lambda dev: branch_all.at[dev], bd_send, bd_recv)

    local[0].wait()
    t_ring.first()
    t_share.give(0, 0, used=False)
    local[1].wait()
    p1_ring.first()
    p1_share.give(0, 0, used=False)
    for i in range(4):
        local[7 + 2 * i].wait()

    def unit_rows(dist, way):
        at = block_of(dist, way) // 2
        x = rows_all[pl.ds(at * 2, 2), :, 0:width].astype(F32).reshape(2 * rows, width)
        mean = jnp.sum(x * x, axis=-1, keepdims=True) * (1.0 / width)
        normed = (x * lax.rsqrt(mean + EPS) * gain_in[...]).astype(BF16)
        got = dot_nt(normed, pin4[...])
        spot = pl.multiple_of(at * (2 * rows), 2 * rows)
        units[pl.ds(spot, 2 * rows), :] = got.astype(BF16).astype(F32)

    def phase1(step, last=False):
        for q in range(t_ring.count):
            for way in (0, 1):
                t_ring.piece(step, way, q, last)
            if q % 2 == 1:
                for way in (0, 1):
                    p1_ring.piece(step, way, q // 2, last)

    def give1(dist, first=False):
        for way in (0, 1):
            t_share.give(dist, way, used=not (first and way == 1))
            p1_share.give(dist, way, used=not (first and way == 1))

    def take1(dist, ways=(0, 1)):
        for way in ways:
            t_share.take(dist, way)
            p1_share.take(dist, way)

    phase1(1, hops == 1)
    give1(1, first=True)
    take1(0, (0,))
    unit_rows(0, 0)

    def body1(step, carry):
        phase1(step)
        give1(step)
        take1(step - 1)
        unit_rows(step - 1, 0)
        unit_rows(step - 1, 1)
        return carry

    lax.fori_loop(2, hops - 1, body1, 0)
    phase1(hops - 1, True)
    give1(hops - 1)
    p2_ring.first()
    take1(hops - 2)
    unit_rows(hops - 2, 0)
    unit_rows(hops - 2, 1)
    take1(hops - 1)
    unit_rows(hops - 1, 0)
    unit_rows(hops - 1, 1)
    t_ring.finish(hops)
    p1_ring.finish(hops)
    t_share.give(hops, 0)
    p1_share.give(hops, 0)

    decay = -params[0:1, :]
    freq = params[1:2, :]
    step_size = jnp.exp(params[2:3, :])
    magnitude = jnp.exp(decay * step_size)
    carry_re = magnitude * jnp.cos(freq * step_size)
    carry_im = magnitude * jnp.sin(freq * step_size)
    denom = decay * decay + freq * freq
    feed_re = ((carry_re - 1.0) * decay + carry_im * freq) / denom
    feed_im = (carry_im * decay - (carry_re - 1.0) * freq) / denom
    same = (iota((32, 128), 0) // 16) == (iota((32, 128), 1) // 64)

    def spread(ref):
        return jnp.where(same, jnp.concatenate([ref[...], ref[...]], axis=1), 0.0)

    w_in_re, w_in_im = spread(in_re), spread(in_im)
    eff_re = feed_re * w_in_re - feed_im * w_in_im
    eff_im = feed_re * w_in_im + feed_im * w_in_re
    zeros = jnp.zeros((96, 128), F32)
    eff_re = jnp.concatenate([eff_re, zeros], axis=0).T.astype(BF16)
    eff_im = jnp.concatenate([eff_im, zeros], axis=0).T.astype(BF16)
    col_re = jnp.broadcast_to(carry_re, (128, 128)).T[:, 0:1]
    col_im = jnp.broadcast_to(carry_im, (128, 128)).T[:, 0:1]
    col_skip = jnp.broadcast_to(params[3:4, :], (128, 128)).T[:, 0:1]
    w_out = jnp.concatenate([spread(out_re), -spread(out_im)], axis=1)
    w_out = jnp.concatenate([w_out] * 4, axis=0).astype(BF16)

    t_share.take(hops, 0)
    p1_share.take(hops, 0)
    unit_rows(hops, 0)
    t_share.close(hops)
    p1_share.close(hops)
    local[2].wait()
    local[3].wait()

    lane_slot = iota((block, 128), 1) // 32
    packed = jnp.zeros((block, 128), F32)
    for r in range(4):
        at = slice(r * block, (r + 1) * block)
        u = units[at, :].T
        u16 = u.astype(BF16)
        old_re, old_im = s_re[:, at], s_im[:, at]
        fresh_re = col_re * old_re - col_im * old_im + dot(eff_re, u16)
        fresh_im = col_re * old_im + col_im * old_re + dot(eff_im, u16)
        o_re[:, at] = fresh_re
        o_im[:, at] = fresh_im
        both = jnp.concatenate([fresh_re, fresh_im], axis=0).astype(BF16)
        read = jax.nn.gelu(dot(w_out, both) + col_skip * u)
        packed = jnp.where(lane_slot == (r + me) % 4, read.T, packed)
    branch_all[me] = packed.astype(BF16)

    b_ring.first()
    b_share.give(0, 0, used=False)
    p2_share.give(0, 0, used=False)
    outs = [
        pltpu.make_async_copy(o_re, new_re, out_sem.at[0]),
        pltpu.make_async_copy(o_im, new_im, out_sem.at[1]),
    ]
    for c in outs:
        c.start()

    def phase2(step, last=False):
        for q in range(2):
            for way in (0, 1):
                p2_ring.piece(step, way, q, last)
            for way in (0, 1):
                b_ring.piece(step, way, q, last)

    def give2(dist, first=False):
        for way in (0, 1):
            b_share.give(dist, way, used=not (first and way == 1))
            p2_share.give(dist, way, used=not (first and way == 1))

    def take2(dist, ways=(0, 1)):
        for way in ways:
            b_share.take(dist, way)
            p2_share.take(dist, way)

    phase2(1, hops == 1)
    give2(1, first=True)
    take2(0, (0,))

    def body2(step, carry):
        phase2(step)
        give2(step)
        take2(step - 1)
        return carry

    lax.fori_loop(2, hops - 1, body2, 0)
    phase2(hops - 1, True)
    give2(hops - 1)
    take2(hops - 2)
    take2(hops - 1)
    p2_ring.finish(hops)
    b_ring.finish(hops)
    b_share.give(hops, 0)
    p2_share.give(hops, 0)
    b_share.take(hops, 0)
    p2_share.take(hops, 0)
    b_share.close(hops)
    p2_share.close(hops)

    for r in range(4):
        for k in range(n // 4):
            got = jnp.zeros((block, 128), F32)
            for i in range(4):
                got = jnp.where(lane_slot == (r + i) % 4, branch_all[4 * k + i].astype(F32), got)
            if r:
                got = pltpu.roll(got, 128 - 32 * r, 1)
            lhs_all[r * block : (r + 1) * block, 128 * k : 128 * k + 128] = got.astype(BF16)

    local[15].wait()
    local[16].wait()
    lane = iota((block, 128), 1)
    mix = params[4:5, :]
    mix_hi = mix.astype(BF16)
    mix_lo = (mix - mix_hi.astype(F32)).astype(BF16)
    mix_rows = jnp.where(
        iota((16, 128), 0) == 0,
        jnp.broadcast_to(mix_hi.astype(F32), (16, 128)),
        jnp.where(iota((16, 128), 0) == 1, jnp.broadcast_to(mix_lo.astype(F32), (16, 128)), 0.0),
    ).astype(BF16)
    wide = min(512, width)

    def mix_block(r, carry):
        base = pl.multiple_of(r * block, block)

        def part(j, c):
            cols = pl.ds(pl.multiple_of(j * wide, wide), wide)
            whole = proj_all[:, :, cols].reshape(n * 32, wide)
            x = rows_all[pl.ds(r * per_block, per_block), :, cols].astype(F32).reshape(block, wide)
            resid[:, cols] = x + dot(lhs_all[pl.ds(base, block), :], whole)
            return c

        lax.fori_loop(0, width // wide, part, 0)

        @pl.when(me // per_block == r)
        def _():
            own_res[...] = resid[pl.ds(pl.multiple_of((me % per_block) * rows, rows), rows), :]

        res = resid[...]
        mean = jnp.sum(res * res, axis=-1, keepdims=True) * (1.0 / width)
        m16 = (res * lax.rsqrt(mean + EPS) * gain_mid[...]).astype(BF16)
        mixed[pl.ds(base, block), :] = m16
        gu = dot_nt(m16, dense_gu[...])
        hid = jnp.where(lane < 64, jax.nn.silu(gu) * pltpu.roll(gu, 64, 1), 0.0).astype(BF16)
        hidden[pl.ds(base, block), :] = hid
        row = jnp.sum(dot_nt(mix_rows, hid), axis=0, keepdims=True)
        logit_all[me, :, pl.ds(base, block)] = row
        return carry

    lax.fori_loop(0, 4, mix_block, 0)

    def logit_copy(j):
        to = (me + j) % n
        return pltpu.make_async_remote_copy(
            src_ref=logit_all.at[me],
            dst_ref=logit_all.at[me],
            send_sem=l_send.at[j],
            recv_sem=l_recv.at[j],
            device_id={"ep": to},
            device_id_type=MESH,
        )

    def logit_arrival(j):
        source = (me - j + n) % n
        return pltpu.make_async_remote_copy(
            src_ref=logit_all.at[source],
            dst_ref=logit_all.at[source],
            send_sem=l_send.at[j],
            recv_sem=l_recv.at[j],
            device_id={"ep": source},
            device_id_type=MESH,
        )

    def send_logit(j, carry):
        logit_copy(j).start()
        return carry

    lax.fori_loop(1, n, send_logit, 0)

    def chosen(r):
        extra = rows_all[pl.ds(r * per_block, per_block), :, width : width + 128]
        extra = extra.astype(F32).reshape(block, 128)
        weight = jnp.sum(
            jnp.where((lane == me) | (lane == n + me), extra, 0.0), axis=-1, keepdims=True
        )
        spot = jnp.sum(jnp.where(lane == 2 * n + me, extra, 0.0), axis=-1, keepdims=True)
        source = (iota((block, 1), 0) // rows).astype(F32)
        slot = jnp.where(spot > 0.5, source * cap + spot - 1.0, -1.0)
        return weight, slot

    lane_f = lane.astype(F32)
    for r in range(4):
        _, slot = chosen(r)
        hot = jnp.where(lane_f == slot, 1.0, 0.0).T.astype(BF16)
        picked[r * slots : (r + 1) * slots, :] = dot(
            hot[0:slots, :], mixed[r * block : (r + 1) * block, :]
        ).astype(BF16)
    local[4].wait()
    local[5].wait()
    local[6].wait()
    fcut = min(256, ff)

    def up_part(j, carry):
        cols = pl.ds(pl.multiple_of(j * fcut, fcut), fcut)
        gated = jnp.minimum(dot(picked[...], w_gate[:, cols]), LIMIT)
        up = jnp.clip(dot(picked[...], w_up[:, cols]), -LIMIT, LIMIT)
        active[:, cols] = ((up + 1.0) * gated * jax.nn.sigmoid(ALPHA * gated)).astype(BF16)
        return carry

    lax.fori_loop(0, ff // fcut, up_part, 0)
    for i in range(4):
        local[8 + 2 * i].wait()

    def down_part(j, carry):
        cols = pl.ds(pl.multiple_of(j * wide, wide), wide)
        out = dot(active[...], w_down[:, cols]).astype(BF16)
        for r in range(4):
            down_rhs[r, 64 : 64 + slots, cols] = out[r * slots : (r + 1) * slots, :]
        return carry

    lax.fori_loop(0, width // wide, down_part, 0)

    def take_logit(j, carry):
        logit_arrival(j).wait_recv()
        logit_copy(j).wait_send()
        return carry

    lax.fori_loop(1, n, take_logit, 0)
    gate_row = jax.nn.sigmoid(jnp.sum(logit_all[...], axis=0))

    def hand_over(r):
        ref = combined.at[other, pl.ds(r * (chips // 4), chips // 4)]
        return pltpu.make_async_remote_copy(
            src_ref=ref,
            dst_ref=partner_part.at[pl.ds(r * (chips // 4), chips // 4)],
            send_sem=cd_send.at[r],
            recv_sem=cd_recv.at[r],
            device_id={"ep": partner},
            device_id_type=MESH,
        )

    for r in range(4):
        at = slice(r * block, (r + 1) * block)
        gate = jnp.broadcast_to(gate_row[:, at], (128, block)).T
        weight, slot = chosen(r)
        lhs = jnp.where(
            lane < 64,
            gate * hidden[at, :].astype(F32),
            jnp.where(lane_f == slot + 64.0, jnp.where(slot >= 0.0, weight, 0.0), 0.0),
        )
        lhs = lhs[:, 0 : 64 + slots].astype(BF16)

        def spread_part(j, carry, r=r, lhs=lhs):
            cols = pl.ds(pl.multiple_of(j * wide, wide), wide)
            out = dot(lhs, down_rhs[r, :, cols]).astype(BF16)
            out = out.reshape(per_block // 2, 2, rows, wide)
            for c in range(2):
                combined[c, pl.ds(r * (chips // 4), chips // 4), :, cols] = out[:, c]
            return carry

        lax.fori_loop(0, width // wide, spread_part, 0)
        hand_over(r).start()

    for r in range(4):
        hand_over(r).wait_recv()

    pieces = [(a, b) for a in range(2) for b in range(2)]

    def rs_copy(step, way, q):
        a, b = pieces[q]
        return pltpu.make_async_remote_copy(
            src_ref=ring_out.at[way, step, pl.ds(a * half_rows, half_rows), pl.ds(b * half_w, half_w)],
            dst_ref=ring_in.at[way, step, pl.ds(a * half_rows, half_rows), pl.ds(b * half_w, half_w)],
            send_sem=r_send.at[way, q],
            recv_sem=r_recv.at[way, step, q],
            device_id={"ep": nexts[way]},
            device_id_type=MESH,
        )

    def rs_own(dist, way, q):
        a, b = pieces[q]
        to = (chip + dist) % chips if way == 0 else (chip - dist + chips) % chips
        rr, cc = pl.ds(a * half_rows, half_rows), pl.ds(b * half_w, half_w)
        return combined[core, to, rr, cc].astype(F32) + partner_part[to, rr, cc].astype(F32)

    def rs_step(step, way, q, got, used):
        a, b = pieces[q]
        rr, cc = pl.ds(a * half_rows, half_rows), pl.ds(b * half_w, half_w)
        value = rs_own(hops - step, way, q)
        if got:
            rs_copy(step - 1, way, q).wait_recv()
            value = value + ring_in[way, step - 1, rr, cc].astype(F32)
        if used:
            rs_copy(step - 1, way, q).wait_send()
        ring_out[way, step, rr, cc] = value.astype(BF16)
        rs_copy(step, way, q).start()

    halves = (range(0, 2), range(2, 4))
    for i in range(2):
        for way in (0, 1):
            rs_step(0, way, halves[way][i], False, False)
    for i in range(2):
        for way in (0, 1):
            rs_step(1, way, halves[1 - way][i], False, False)
    for i in range(2):
        for way in (0, 1):
            rs_step(1, way, halves[way][i], True, True)

    def rs_body(step, carry):
        for q in range(4):
            for way in (0, 1):
                rs_step(step, way, q, True, True)
        return carry

    lax.fori_loop(2, hops, rs_body, 0)
    for q in range(4):
        a, b = pieces[q]
        rr, cc = pl.ds(a * half_rows, half_rows), pl.ds(b * half_w, half_w)
        value = rs_own(0, 0, q) + own_res[rr, cc]
        for way in (0, 1):
            rs_copy(hops - 1, way, q).wait_recv()
            value = value + ring_in[way, hops - 1, rr, cc].astype(F32)
        layer_out[rr, cc] = value.astype(BF16)
    for q in range(4):
        for way in (0, 1):
            rs_copy(hops - 1, way, q).wait_send()
    for r in range(4):
        hand_over(r).wait_send()
    for c in outs:
        c.wait()


def on_device(
    tokens,
    routes,
    route_logits,
    state_real,
    state_imag,
    gain_in,
    proj_in,
    decay_rate,
    frequency,
    log_step,
    input_real,
    input_imag,
    output_real,
    output_imag,
    skip_gain,
    proj_out,
    gain_mid,
    expert_gate,
    expert_up,
    expert_down,
    dense_gate,
    dense_up,
    dense_down,
    dense_mix,
):
    n = lax.axis_size("ep")
    rows, width = tokens.shape
    top = routes.shape[1]
    ff = expert_gate.shape[2]
    seqs = state_real.shape[0]
    cap = max(2, 2 * rows * top // n)
    chips, hops, block = n // 2, n // 4, seqs // 4
    slots = (n // 4) * cap
    params = jnp.stack(
        [
            decay_rate.reshape(128),
            frequency.reshape(128),
            jnp.repeat(log_step, 64),
            jnp.tile(skip_gain.reshape(32), 4),
            jnp.pad(dense_mix, (0, 64)),
        ]
    )
    operands = (
        tokens,
        routes.T,
        route_logits.T,
        state_real.transpose(1, 2, 0).reshape(128, seqs),
        state_imag.transpose(1, 2, 0).reshape(128, seqs),
        gain_in[None],
        proj_in.T,
        params,
        input_real.transpose(0, 2, 1).reshape(32, 64),
        input_imag.transpose(0, 2, 1).reshape(32, 64),
        output_real.reshape(32, 64),
        output_imag.reshape(32, 64),
        proj_out,
        gain_mid[None],
        expert_gate[0],
        expert_up[0],
        expert_down[0],
        dense_gate.T,
        dense_up.T,
        dense_down,
    )
    vmem = pl.BlockSpec(memory_space=pltpu.VMEM)
    far = pl.BlockSpec(memory_space=pl.ANY)
    in_specs = [
        far,
        vmem,
        vmem,
        far,
        far,
        vmem,
        far,
        vmem,
        vmem,
        vmem,
        vmem,
        vmem,
        far,
        vmem,
        far,
        far,
        far,
        far,
        far,
        far,
    ]
    V = pltpu.VMEM
    dma = pltpu.SemaphoreType.DMA
    scratch = [
        V((n, rows, width + 128), BF16),
        V((n, 32, width), BF16),
        V((n, block, 128), BF16),
        V((seqs, n * 32), BF16),
        V((block, width), F32),
        V((rows, width), F32),
        V((seqs, width), BF16),
        V((width, ff), BF16),
        V((width, ff), BF16),
        V((ff, width), BF16),
        V((128, seqs), F32),
        V((128, seqs), F32),
        V((128, seqs), F32),
        V((128, seqs), F32),
        V((4 * slots, width), BF16),
        V((4 * slots, ff), BF16),
        V((4, 64 + slots, width), BF16),
        V((2, chips, rows, width), BF16),
        V((chips, rows, width), BF16),
        V((2, hops, rows, width), BF16),
        V((2, hops, rows, width), BF16),
        V((seqs, 128), F32),
        V((128, width), BF16),
        V((128, width), BF16),
        V((seqs, 128), BF16),
        V((n, 1, seqs), F32),
        V((128, 128), F32),
        dma((17,)),
        dma((2,)),
        dma((2, 4)),
        dma((2, hops, 4)),
        dma((2, 2)),
        dma((2, hops, 2)),
        dma((2, 2)),
        dma((2, hops, 2)),
        dma((2, 2)),
        dma((2, hops, 2)),
        dma((2, 4)),
        dma((2, hops, 4)),
    ]
    for _ in range(4):
        scratch += [dma((2,)), dma((2, hops + 1))]
    scratch += [dma((4,)), dma((4,)), dma((n,)), dma((n,))]
    layer_out, new_re, new_im = pl.pallas_call(
        functools.partial(kernel, n, (rows, width, ff, cap)),
        out_shape=(
            jax.ShapeDtypeStruct((rows, width), BF16),
            jax.ShapeDtypeStruct((128, seqs), F32),
            jax.ShapeDtypeStruct((128, seqs), F32),
        ),
        in_specs=in_specs,
        out_specs=(vmem, far, far),
        scratch_shapes=scratch,
        compiler_params=pltpu.CompilerParams(
            collective_id=0, has_side_effects=True, vmem_limit_bytes=66_000_000
        ),
        name="layer_step",
    )(*operands)
    groups, state = state_real.shape[1:]

    def back(values):
        return values.reshape(groups, state, seqs).transpose(2, 0, 1)

    return (layer_out, back(new_re), back(new_im))


def solution(mesh):
    both = ("grp", "ep")
    return jax.shard_map(
        on_device,
        mesh=mesh,
        in_specs=(
            P(both, None),
            P(both, None),
            P(both, None),
            P("grp", "ep", None),
            P("grp", "ep", None),
            P(),
            P(None, "ep"),
            P("ep", None),
            P("ep", None),
            P("ep"),
            P("ep", None, None),
            P("ep", None, None),
            P("ep", None, None),
            P("ep", None, None),
            P("ep", None),
            P("ep", None),
            P(),
            P("ep", None, None),
            P("ep", None, None),
            P("ep", None, None),
            P(None, "ep"),
            P(None, "ep"),
            P("ep", None),
            P("ep"),
        ),
        out_specs=(P(both, None), P("grp", "ep", None), P("grp", "ep", None)),
        check_vma=False,
    )
```

```python
import functools

import jax
import jax.numpy as jnp
from jax import lax
from jax.experimental import pallas as pl
from jax.experimental.pallas import tpu as pltpu
from jax.sharding import PartitionSpec as P

EPS = 1e-06
LIMIT = 7.0
ALPHA = 1.702
MESH = pl.DeviceIdType.MESH
F32 = jnp.float32
BF16 = jnp.bfloat16
NT = (((1,), (1,)), ((), ()))


def dot(a, b):
    return jnp.dot(a, b, preferred_element_type=F32)


def dot_nt(a, b):
    return lax.dot_general(a, b, NT, preferred_element_type=F32)


def iota(shape, dim):
    return lax.broadcasted_iota(jnp.int32, shape, dim)


class Ring:
    def __init__(self, pieces, send, recv, where):
        self.pieces, self.send, self.recv, self.where = pieces, send, recv, where
        self.count = len(pieces)

    def copy(self, step, way, q):
        ref = self.pieces[q](self.where["block"](step, way))
        return pltpu.make_async_remote_copy(
            src_ref=ref,
            dst_ref=ref,
            send_sem=self.send.at[way, q],
            recv_sem=self.recv.at[way, step, q],
            device_id={"ep": self.where["next"][way]},
            device_id_type=MESH,
        )

    def arrival(self, step, way, q):
        ref = self.pieces[q](self.where["block"](step + 1, way))
        return pltpu.make_async_remote_copy(
            src_ref=ref,
            dst_ref=ref,
            send_sem=self.send.at[way, q],
            recv_sem=self.recv.at[way, step, q],
            device_id={"ep": self.where["next"][way]},
            device_id_type=MESH,
        )

    def half(self, way):
        mid = self.count // 2
        return range(mid) if way == 0 else range(mid, self.count)

    def first(self):
        for q in range(self.count):
            for way in (0, 1):
                self.copy(0, way, q).start()

    def piece(self, step, way, q, last=False):
        self.arrival(step - 1, way, q).wait_recv()
        self.copy(step - 1, way, q).wait_send()
        if not last or q in self.half(way):
            self.copy(step, way, q).start()

    def finish(self, hops):
        for way in (0, 1):
            for q in self.half(way):
                self.arrival(hops - 1, way, q).wait_recv()
                self.copy(hops - 1, way, q).wait_send()


def kernel(
    n,
    dims,
    tokens,
    routes_t,
    logits_t,
    state_re,
    state_im,
    gain_in,
    proj_in_t,
    decay_rate,
    frequency,
    log_step,
    skip_gain,
    dense_mix,
    in_re,
    in_im,
    out_re,
    out_im,
    proj_out,
    gain_mid,
    expert_gate,
    expert_up,
    expert_down,
    dense_gate_t,
    dense_up_t,
    dense_down,
    layer_out,
    new_re,
    new_im,
    rows_all,
    proj_all,
    branch_all,
    total,
    mixed,
    w_gate,
    w_up,
    w_down,
    s_re,
    s_im,
    o_re,
    o_im,
    picked,
    final_lhs,
    active,
    down_rhs,
    combined,
    partner_part,
    ring_in,
    ring_out,
    units,
    pin4,
    dense_gu,
    spread_lhs,
    scale_all,
    logit_pair,
    logit_all,
    square,
    local_sem,
    out_sem,
    t_send,
    p1_send,
    p2_send,
    b_send,
    r_send,
    recv_a,
    recv_b,
    td_send,
    p1d_send,
    p2d_send,
    bd_send,
    share_a,
    share_b,
    cd_send,
    cd_recv,
    l_send,
    l_recv,
    lp_send,
    lp_recv,
):
    rows, width, ff, cap = dims
    chips = n // 2
    hops = chips // 2
    seqs = n * rows
    block = seqs // 4
    per_block = n // 4
    slots = per_block * cap
    me = lax.axis_index("ep")
    chip = me // 2
    core = me % 2
    other = 1 - core
    partner = chip * 2 + other
    right = ((chip + 1) % chips) * 2 + core
    left = ((chip + chips - 1) % chips) * 2 + core
    nexts = (right, left)

    def block_of(step, way):
        at = (chip - step + chips) % chips if way == 0 else (chip + step) % chips
        return at * 2 + core

    where = {"next": nexts, "block": block_of}

    half_rows = rows // 2
    local = [
        pltpu.make_async_copy(tokens, rows_all.at[me, :, pl.ds(0, width)], local_sem.at[0]),
        pltpu.make_async_copy(proj_out, proj_all.at[me], local_sem.at[1]),
        pltpu.make_async_copy(state_re, s_re, local_sem.at[2]),
        pltpu.make_async_copy(state_im, s_im, local_sem.at[3]),
        pltpu.make_async_copy(expert_gate, w_gate, local_sem.at[4]),
        pltpu.make_async_copy(expert_up, w_up, local_sem.at[5]),
        pltpu.make_async_copy(expert_down, w_down, local_sem.at[6]),
    ]
    for i in range(4):
        local.append(pltpu.make_async_copy(proj_in_t, pin4.at[pl.ds(32 * i, 32)], local_sem.at[7 + i]))
        local.append(pltpu.make_async_copy(dense_down, down_rhs.at[i, pl.ds(0, 64)], local_sem.at[11 + i]))
    local.append(pltpu.make_async_copy(dense_gate_t, dense_gu.at[pl.ds(0, 64)], local_sem.at[15]))
    local.append(pltpu.make_async_copy(dense_up_t, dense_gu.at[pl.ds(64, 64)], local_sem.at[16]))
    for i in (0, 1, 7, 9, 11, 13):
        local[i].start()

    barrier = pltpu.get_barrier_semaphore()
    for peer in (left, right, partner):
        pl.semaphore_signal(barrier, inc=1, device_id={"ep": peer}, device_id_type=MESH)

    expert_row = iota((128, rows), 0)
    expert_id = expert_row % n
    scores = jnp.exp(logits_t[...])
    scores = scores / jnp.sum(scores, axis=0, keepdims=True)
    top = scores.shape[0]
    share = jnp.zeros((128, rows), F32)
    for k in range(top):
        share = share + jnp.where(routes_t[k : k + 1, :] == expert_id, scores[k : k + 1, :], 0.0)
    mark = jnp.where(share > 0.0, 1.0, 0.0)
    upper = jnp.where(iota((rows, rows), 0) <= iota((rows, rows), 1), 1.0, 0.0)
    rank = dot(mark.astype(BF16), upper.astype(BF16)) * mark
    part_hi = share.astype(BF16).astype(F32)
    kind = expert_row // n
    extra = jnp.where(
        kind == 0, part_hi, jnp.where(kind == 1, share - part_hi, jnp.where(kind == 2, rank, 0.0))
    )
    square[...] = jnp.zeros(square.shape, F32)
    square[:, 0:rows] = extra
    rows_all[me, :, width : width + 128] = square[...].T[0:rows, :].astype(BF16)

    pl.semaphore_wait(barrier, 3)

    ext = width + 128
    cut = ((ext // 128 + 1) // 2) * 128
    half_w = width // 2

    def row_piece(r0, c0, c1):
        return lambda dev: rows_all.at[dev, pl.ds(r0, half_rows), pl.ds(c0, c1 - c0)]

    def proj_piece(r0, c0, size):
        return lambda dev: proj_all.at[dev, pl.ds(r0, half_rows), pl.ds(c0, size)]

    def branch_piece(r0):
        return lambda dev: branch_all.at[dev, pl.ds(r0, block // 4)]

    t_ring = Ring(
        [
            row_piece(0, 0, cut),
            row_piece(0, cut, ext),
            row_piece(half_rows, 0, cut),
            row_piece(half_rows, cut, ext),
        ],
        t_send,
        recv_a,
        where,
    )
    p1_ring = Ring([proj_piece(0, 0, half_w), proj_piece(0, half_w, half_w)], p1_send, recv_b, where)
    p2_ring = Ring(
        [proj_piece(half_rows, i * (width // 4), width // 4) for i in range(4)], p2_send, recv_b, where
    )
    b_ring = Ring([branch_piece(i * (block // 4)) for i in range(4)], b_send, recv_a, where)

    class Share:
        def __init__(self, ref, send, recv):
            self.ref, self.send, self.recv = ref, send, recv

        def copy(self, dist, way, which):
            ref = self.ref(block_of(dist, way) // 2 * 2 + which)
            return pltpu.make_async_remote_copy(
                src_ref=ref,
                dst_ref=ref,
                send_sem=self.send.at[way],
                recv_sem=self.recv.at[way, dist],
                device_id={"ep": partner},
                device_id_type=MESH,
            )

        def give(self, dist, way, used=True):
            if used:
                self.copy(dist, way, core).wait_send()
            self.copy(dist, way, core).start()

        def take(self, dist, way):
            self.copy(dist, way, other).wait_recv()

        def close(self, dist):
            for way in (0, 1):
                self.copy(dist, way, core).wait_send()

    t_share = Share(lambda dev: rows_all.at[dev], td_send, share_a)
    p1_share = Share(lambda dev: proj_all.at[dev, pl.ds(0, half_rows)], p1d_send, share_b)
    p2_share = Share(lambda dev: proj_all.at[dev, pl.ds(half_rows, half_rows)], p2d_send, share_b)
    b_share = Share(lambda dev: branch_all.at[dev], bd_send, share_a)

    local[0].wait()
    t_ring.first()
    t_share.give(0, 0, used=False)
    local[1].wait()
    p1_ring.first()
    p1_share.give(0, 0, used=False)
    for i in range(17):
        if i not in (0, 1, 7, 9, 11, 13):
            local[i].start()
    for i in range(4):
        local[7 + 2 * i].wait()

    def unit_rows(dist, way):
        at = block_of(dist, way) // 2
        x = rows_all[pl.ds(at * 2, 2), :, 0:width].astype(F32).reshape(2 * rows, width)
        mean = jnp.sum(x * x, axis=-1, keepdims=True) * (1.0 / width)
        normed = (x * lax.rsqrt(mean + EPS) * gain_in[...]).astype(BF16)
        got = dot_nt(normed, pin4[...])
        spot = pl.multiple_of(at * (2 * rows), 2 * rows)
        total[pl.ds(spot, 2 * rows), :] = x
        units[pl.ds(spot, 2 * rows), :] = got.astype(BF16).astype(F32)

    def phase1(step, last=False):
        for q in range(t_ring.count):
            for way in (0, 1):
                t_ring.piece(step, way, q, last)
            if q % 2 == 1:
                for way in (0, 1):
                    p1_ring.piece(step, way, q // 2, last)

    def give1(dist, first=False):
        for way in (0, 1):
            t_share.give(dist, way, used=not (first and way == 1))
            p1_share.give(dist, way, used=not (first and way == 1))

    def take1(dist, ways=(0, 1)):
        for way in ways:
            t_share.take(dist, way)
            p1_share.take(dist, way)

    phase1(1, hops == 1)
    give1(1, first=True)
    take1(0, (0,))
    unit_rows(0, 0)

    def body1(step, carry):
        phase1(step)
        give1(step)
        take1(step - 1)
        unit_rows(step - 1, 0)
        unit_rows(step - 1, 1)
        return carry

    lax.fori_loop(2, hops - 1, body1, 0)
    phase1(hops - 1, True)
    give1(hops - 1)
    p2_ring.first()
    p2_share.give(0, 0, used=False)
    take1(hops - 2)
    unit_rows(hops - 2, 0)
    unit_rows(hops - 2, 1)
    take1(hops - 1)
    unit_rows(hops - 1, 0)
    unit_rows(hops - 1, 1)
    t_ring.finish(hops)
    p1_ring.finish(hops)
    t_share.give(hops, 0)
    p1_share.give(hops, 0)

    def flat(ref):
        return jnp.concatenate([ref[0:1, :], ref[1:2, :]], axis=1)

    decay = -flat(decay_rate)
    freq = flat(frequency)
    step_size = jnp.exp(jnp.where(iota((1, 128), 1) < 64, log_step[0:1, 0:1], log_step[0:1, 1:2]))
    magnitude = jnp.exp(decay * step_size)
    carry_re = magnitude * jnp.cos(freq * step_size)
    carry_im = magnitude * jnp.sin(freq * step_size)
    denom = decay * decay + freq * freq
    feed_re = ((carry_re - 1.0) * decay + carry_im * freq) / denom
    feed_im = (carry_im * decay - (carry_re - 1.0) * freq) / denom
    same = (iota((32, 128), 0) // 16) == (iota((32, 128), 1) // 64)

    def spread(ref):
        return jnp.where(same, jnp.concatenate([ref[...], ref[...]], axis=1), 0.0)

    w_in_re, w_in_im = spread(in_re), spread(in_im)
    eff_re = feed_re * w_in_re - feed_im * w_in_im
    eff_im = feed_re * w_in_im + feed_im * w_in_re
    zeros = jnp.zeros((96, 128), F32)
    eff_re = jnp.concatenate([eff_re, zeros], axis=0).T.astype(BF16)
    eff_im = jnp.concatenate([eff_im, zeros], axis=0).T.astype(BF16)
    col_re = jnp.broadcast_to(carry_re, (128, 128)).T[:, 0:1]
    col_im = jnp.broadcast_to(carry_im, (128, 128)).T[:, 0:1]
    skip_row = iota((128, 16), 0) % 32
    skips = jnp.where(skip_row < 16, skip_gain[0:1, :], skip_gain[1:2, :])
    col_skip = jnp.sum(
        jnp.where(skip_row % 16 == iota((128, 16), 1), skips, 0.0), axis=1, keepdims=True
    )
    w_out = jnp.concatenate([spread(out_re), -spread(out_im)], axis=1)
    w_out = jnp.concatenate([w_out] * 4, axis=0).astype(BF16)

    t_share.take(hops, 0)
    p1_share.take(hops, 0)
    unit_rows(hops, 0)
    t_share.close(hops)
    p1_share.close(hops)
    local[2].wait()
    local[3].wait()

    def p2_step(step, last=False):
        for q in range(4):
            for way in (0, 1):
                p2_ring.piece(step, way, q, last)
        p2_share.give(step, 0)
        p2_share.give(step, 1, used=step > 1) if isinstance(step, int) else p2_share.give(step, 1)

    p2_step(1)
    lane_slot = iota((block, 128), 1) // 32
    packed = jnp.zeros((block, 128), F32)
    for r in range(4):
        at = slice(r * block, (r + 1) * block)
        u = units[at, :].T
        u16 = u.astype(BF16)
        old_re, old_im = s_re[:, at], s_im[:, at]
        fresh_re = col_re * old_re - col_im * old_im + dot(eff_re, u16)
        fresh_im = col_re * old_im + col_im * old_re + dot(eff_im, u16)
        o_re[:, at] = fresh_re
        o_im[:, at] = fresh_im
        both = jnp.concatenate([fresh_re, fresh_im], axis=0).astype(BF16)
        read = jax.nn.gelu(dot(w_out, both) + col_skip * u)
        packed = jnp.where(lane_slot == (r + me) % 4, read.T, packed)
    branch_all[me] = packed.astype(BF16)

    b_ring.first()
    b_share.give(0, 0, used=False)
    outs = [
        pltpu.make_async_copy(o_re, new_re, out_sem.at[0]),
        pltpu.make_async_copy(o_im, new_im, out_sem.at[1]),
    ]
    for c in outs:
        c.start()

    wide = min(512, width)

    def pair_of(k):
        a, b = block_of(k, 0) // 2, block_of(k + 1, 1) // 2
        even = jnp.where(a % 2 == 0, a, b)
        return even, a + b - even

    def pair_lhs(k, r):
        even, odd = pair_of(k)
        got = branch_all[2 * even].astype(F32)
        for i, dev in ((1, 2 * even + 1), (2, 2 * odd), (3, 2 * odd + 1)):
            got = jnp.where(lane_slot == (r + i) % 4, branch_all[dev].astype(F32), got)
        return pltpu.roll(got, (128 - 32 * r) % 128, 1).astype(BF16)

    def quad_lhs(j, r):
        return jnp.concatenate([pair_lhs(2 * j, r), pair_lhs(2 * j + 1, r)], axis=1)

    def quad_rhs(j, cols):
        chips4 = pair_of(2 * j) + pair_of(2 * j + 1)
        return jnp.concatenate(
            [proj_all[pl.ds(2 * at, 2), :, cols].reshape(64, wide) for at in chips4], axis=0
        )

    def mix_rows(j, r):
        at = pl.ds(pl.multiple_of(r * block, block), block)
        lhs = quad_lhs(j, r)
        for c in range(width // wide):
            cols = slice(c * wide, (c + 1) * wide)
            total[at, cols] = total[at, cols] + dot(lhs, quad_rhs(j, cols))

    def take2(dist):
        for way in (0,) if isinstance(dist, int) and dist in (0, hops) else (0, 1):
            b_share.take(dist, way)
            p2_share.take(dist, way)

    def b_step(step, p2_next, last=False, p2_last=False):
        for q in range(4):
            for way in (0, 1):
                if p2_next is not None:
                    p2_ring.piece(p2_next, way, q, p2_last)
                b_ring.piece(step, way, q, last)
            if isinstance(step, int) and step < 3:
                continue
            if q == 0:
                take2(step - 1)
            if q % 2 == 1:
                turn = step - 3
                mix_rows(turn // 2, turn % 2 * 2 + q // 2)
        first = isinstance(step, int) and step == 1
        for way in (0, 1):
            if p2_next is not None:
                p2_share.give(p2_next, way)
            b_share.give(step, way, used=not (first and way == 1))

    b_step(1, 2)
    take2(0)
    b_step(2, 3, p2_last=hops == 4)
    take2(1)

    def body2(step, carry):
        b_step(step, step + 1)
        return carry

    lax.fori_loop(3, hops - 2, body2, 0)
    if hops > 4:
        b_step(hops - 2, hops - 1, p2_last=True)
    b_step(hops - 1, None, last=True)
    p2_ring.finish(hops)
    p2_share.give(hops, 0)
    take2(hops - 1)
    mix_rows(hops // 2 - 2, 2)
    mix_rows(hops // 2 - 2, 3)
    b_ring.finish(hops)
    b_share.give(hops, 0)
    take2(hops)
    b_share.close(hops)
    p2_share.close(hops)

    local[15].wait()
    local[16].wait()
    lane = iota((block, 128), 1)
    lane_f = lane.astype(F32)
    mix = jnp.concatenate([dense_mix[...], jnp.zeros((1, 64), F32)], axis=1)
    mix_hi = mix.astype(BF16).astype(F32)
    row16 = iota((16, 128), 0)
    mix_rows16 = jnp.where(row16 == 0, mix_hi, jnp.where(row16 == 1, mix - mix_hi, 0.0)).astype(BF16)

    for r in range(4):
        at = slice(r * block, (r + 1) * block)
        lhs = quad_lhs(hops // 2 - 1, r)
        squares = jnp.zeros((block, 128), F32)
        for c in range(width // wide):
            cols = slice(c * wide, (c + 1) * wide)
            res = total[at, cols] + dot(lhs, quad_rhs(hops // 2 - 1, cols))
            total[at, cols] = res
            mixed[at, cols] = (res * gain_mid[:, cols]).astype(BF16)
            sq = res * res
            for i in range(wide // 128):
                squares = squares + sq[:, 128 * i : 128 * i + 128]

        scale = lax.rsqrt(jnp.sum(squares, axis=-1, keepdims=True) * (1.0 / width) + EPS)
        scale_all[at, :] = jnp.broadcast_to(scale, (block, 128))
        gu = dot_nt(mixed[at, :], dense_gu[...]) * scale
        hid = jnp.where(lane < 64, jax.nn.silu(gu) * pltpu.roll(gu, 64, 1), 0.0).astype(BF16)
        spread_lhs[at, :] = hid.astype(F32)
        logit_pair[core, :, at] = jnp.sum(dot_nt(mix_rows16, hid), axis=0, keepdims=True)

    def pair_copy(which):
        ref = logit_pair.at[which]
        return pltpu.make_async_remote_copy(
            src_ref=ref,
            dst_ref=ref,
            send_sem=lp_send.at[0],
            recv_sem=lp_recv.at[0],
            device_id={"ep": partner},
            device_id_type=MESH,
        )

    pair_copy(core).start()

    def logit_copy(j):
        return pltpu.make_async_remote_copy(
            src_ref=logit_all.at[me],
            dst_ref=logit_all.at[me],
            send_sem=l_send.at[0],
            recv_sem=l_recv.at[0],
            device_id={"ep": (me + j) % n},
            device_id_type=MESH,
        )

    def logit_rest():
        ref = logit_all.at[pl.ds(0, n - 1)]
        return pltpu.make_async_remote_copy(
            src_ref=ref,
            dst_ref=ref,
            send_sem=l_send.at[0],
            recv_sem=l_recv.at[0],
            device_id={"ep": partner},
            device_id_type=MESH,
        )

    def send_logit(j, carry):
        logit_copy(j).start()
        return carry

    def pick(r):
        at = slice(r * block, (r + 1) * block)
        extra = rows_all[r * per_block : (r + 1) * per_block, :, width : width + 128]
        extra = extra.astype(F32).reshape(block, 128)
        weight = jnp.sum(
            jnp.where((lane == me) | (lane == n + me), extra, 0.0), axis=-1, keepdims=True
        )
        spot = jnp.sum(jnp.where(lane == 2 * n + me, extra, 0.0), axis=-1, keepdims=True)
        source = (iota((block, 1), 0) // rows).astype(F32)
        slot = jnp.where(spot > 0.5, source * cap + spot - 1.0, -128.0)
        hot = jnp.where(lane_f == slot, scale_all[at, :], 0.0).T[0:slots, :]
        picked[r * slots : (r + 1) * slots, :] = dot(
            jnp.where(hot > 0.0, 1.0, 0.0).astype(BF16), mixed[at, :]
        ).astype(BF16)
        scale_all[r * slots : (r + 1) * slots, :] = jnp.broadcast_to(
            jnp.sum(hot, axis=-1, keepdims=True), (slots, 128)
        )
        spread_lhs[at, :] = jnp.where(lane_f == slot + 64.0, weight, spread_lhs[at, :])

    pick(0)
    pick(1)
    pair_copy(other).wait_recv()
    mine = pl.ds(pl.multiple_of(core * (seqs // 2), seqs // 2), seqs // 2)
    logit_all[me] = logit_pair[0, :, mine] + logit_pair[1, :, mine]
    lax.fori_loop(1, n, send_logit, 0)
    pair_copy(core).wait_send()
    pick(2)
    pick(3)
    local[4].wait()
    local[5].wait()
    local[6].wait()
    fcut = min(256, ff)

    def up_part(j, carry):
        cols = pl.ds(pl.multiple_of(j * fcut, fcut), fcut)
        scale = scale_all[0 : 4 * slots, 0:1]
        gated = jnp.minimum(dot(picked[...], w_gate[:, cols]) * scale, LIMIT)
        up = jnp.clip(dot(picked[...], w_up[:, cols]) * scale, -LIMIT, LIMIT)
        active[:, cols] = ((up + 1.0) * gated * jax.nn.sigmoid(ALPHA * gated)).astype(BF16)
        return carry

    lax.fori_loop(0, ff // fcut, up_part, 0)
    for i in range(4):
        local[8 + 2 * i].wait()

    def down_part(j, carry):
        cols = pl.ds(pl.multiple_of(j * wide, wide), wide)
        out = dot(active[...], w_down[:, cols]).astype(BF16)
        for r in range(4):
            down_rhs[r, 64 : 64 + slots, cols] = out[r * slots : (r + 1) * slots, :]
        return carry

    lax.fori_loop(0, width // wide, down_part, 0)

    logit_rest().wait_recv()
    logit_rest().wait_send()
    gates = logit_all[...].reshape(chips, 2, 1, seqs // 2)
    gate_rows = [jax.nn.sigmoid(jnp.sum(gates[:, c], axis=0)) for c in range(2)]
    for r in range(4):
        row = gate_rows[r // 2][:, (r % 2) * block : (r % 2 + 1) * block]
        gate = jnp.broadcast_to(row, (128, block)).T
        at = slice(r * block, (r + 1) * block)
        scaled = jnp.where(lane < 64, gate * spread_lhs[at, :], spread_lhs[at, :])
        final_lhs[r] = scaled.astype(BF16)

    quarter = chips // 4

    def hand_over(r):
        ref = combined.at[other, pl.ds(r * quarter, quarter)]
        return pltpu.make_async_remote_copy(
            src_ref=ref,
            dst_ref=partner_part.at[pl.ds(r * quarter, quarter)],
            send_sem=cd_send.at[r],
            recv_sem=cd_recv.at[r],
            device_id={"ep": partner},
            device_id_type=MESH,
        )

    far_block = ((chip + hops) % chips) // quarter

    def combine(turn):
        r = (far_block + turn) % 4
        lhs = final_lhs[r, :, 0 : 64 + slots]

        for j in range(width // wide):
            cols = slice(j * wide, (j + 1) * wide)
            out = dot(lhs, down_rhs[r, :, cols]).astype(BF16)
            out = out.reshape(quarter, 2, rows, wide)
            for c in range(2):
                combined[c, pl.ds(r * quarter, quarter), :, cols] = out[:, c]
        hand_over(r).start()

    def handed(turn):
        hand_over((far_block + turn) % 4).wait_recv()

    pieces = [(a, b) for a in range(2) for b in range(4)]
    part_w = width // 4

    def rs_copy(step, way, q):
        a, b = pieces[q]
        return pltpu.make_async_remote_copy(
            src_ref=ring_out.at[way, step, pl.ds(a * half_rows, half_rows), pl.ds(b * part_w, part_w)],
            dst_ref=ring_in.at[way, step, pl.ds(a * half_rows, half_rows), pl.ds(b * part_w, part_w)],
            send_sem=r_send.at[way, q],
            recv_sem=(recv_a if q < 4 else recv_b).at[way, step, q % 4],
            device_id={"ep": nexts[way]},
            device_id_type=MESH,
        )

    def rs_own(dist, way, q):
        a, b = pieces[q]
        to = (chip + dist) % chips if way == 0 else (chip - dist + chips) % chips
        rr, cc = pl.ds(a * half_rows, half_rows), pl.ds(b * part_w, part_w)
        return combined[core, to, rr, cc].astype(F32) + partner_part[to, rr, cc].astype(F32)

    def rs_step(step, way, q, got, used):
        a, b = pieces[q]
        rr, cc = pl.ds(a * half_rows, half_rows), pl.ds(b * part_w, part_w)
        value = rs_own(hops - step, way, q)
        if got:
            rs_copy(step - 1, way, q).wait_recv()
            value = value + ring_in[way, step - 1, rr, cc].astype(F32)
        if used:
            rs_copy(step - 1, way, q).wait_send()
        ring_out[way, step, rr, cc] = value.astype(BF16)
        rs_copy(step, way, q).start()

    halves = (range(0, 4), range(4, 8))
    combine(0)
    combine(1)
    handed(0)
    for i in range(4):
        for way in (0, 1):
            rs_step(0, way, halves[way][i], False, False)
    combine(3)
    handed(1)
    handed(3)
    for i in range(4):
        for way in (0, 1):
            rs_step(1, way, halves[1 - way][i], False, False)
    combine(2)
    for i in range(4):
        for way in (0, 1):
            rs_step(1, way, halves[way][i], True, True)
    handed(2)

    def rs_body(step, carry):
        for q in range(8):
            for way in (0, 1):
                rs_step(step, way, q, True, True)
        return carry

    lax.fori_loop(2, hops, rs_body, 0)
    own_rows = pl.ds(pl.multiple_of(me * rows, rows), rows)
    for q in range(8):
        a, b = pieces[q]
        rr, cc = pl.ds(a * half_rows, half_rows), pl.ds(b * part_w, part_w)
        value = rs_own(0, 0, q) + total[own_rows, :][a * half_rows : (a + 1) * half_rows, b * part_w : (b + 1) * part_w]
        for way in (0, 1):
            rs_copy(hops - 1, way, q).wait_recv()
            value = value + ring_in[way, hops - 1, rr, cc].astype(F32)
        layer_out[rr, cc] = value.astype(BF16)
    for q in range(8):
        for way in (0, 1):
            rs_copy(hops - 1, way, q).wait_send()
    for r in range(4):
        hand_over(r).wait_send()
    for c in outs:
        c.wait()


def write_out(sources, targets, buffers, in_sem, out_sem):
    count = len(sources)
    takes = [pltpu.make_async_copy(sources[i], buffers[i], in_sem.at[i]) for i in range(count)]
    gives = [pltpu.make_async_copy(buffers[i], targets[i], out_sem.at[i]) for i in range(count)]
    for take in takes:
        take.start()
    for take, give in zip(takes, gives):
        take.wait()
        give.start()
    for give in gives:
        give.wait()


def finish(a, b, c, out_a, out_b, out_c, va, vb, vc, in_sem, out_sem):
    half = b.shape[0] // 2
    cuts = [pl.ds(0, half), pl.ds(half, half)]
    write_out(
        [b.at[cut] for cut in cuts] + [c.at[cut] for cut in cuts] + [a],
        [out_b.at[cut] for cut in cuts] + [out_c.at[cut] for cut in cuts] + [out_a],
        [vb.at[cut] for cut in cuts] + [vc.at[cut] for cut in cuts] + [va],
        in_sem,
        out_sem,
    )


def on_device(
    tokens,
    routes,
    route_logits,
    state_real,
    state_imag,
    gain_in,
    proj_in,
    decay_rate,
    frequency,
    log_step,
    input_real,
    input_imag,
    output_real,
    output_imag,
    skip_gain,
    proj_out,
    gain_mid,
    expert_gate,
    expert_up,
    expert_down,
    dense_gate,
    dense_up,
    dense_down,
    dense_mix,
):
    n = lax.axis_size("ep")
    rows, width = tokens.shape
    top = routes.shape[1]
    ff = expert_gate.shape[2]
    seqs = state_real.shape[0]
    cap = max(2, 2 * rows * top // n)
    chips, hops, block = n // 2, n // 4, seqs // 4
    slots = (n // 4) * cap
    operands = (
        tokens,
        routes.T,
        route_logits.T,
        state_real.transpose(1, 2, 0).reshape(128, seqs),
        state_imag.transpose(1, 2, 0).reshape(128, seqs),
        gain_in[None],
        proj_in.T,
        decay_rate,
        frequency,
        log_step[None],
        skip_gain,
        dense_mix[None],
        input_real.transpose(0, 2, 1).reshape(32, 64),
        input_imag.transpose(0, 2, 1).reshape(32, 64),
        output_real.reshape(32, 64),
        output_imag.reshape(32, 64),
        proj_out,
        gain_mid[None],
        expert_gate[0],
        expert_up[0],
        expert_down[0],
        dense_gate.T,
        dense_up.T,
        dense_down,
    )
    vmem = pl.BlockSpec(memory_space=pltpu.VMEM)
    far = pl.BlockSpec(memory_space=pl.ANY)
    in_specs = [far] + [vmem] * 2 + [far] * 2 + [vmem, far] + [vmem] * 9 + [far, vmem] + [far] * 6
    V = pltpu.VMEM
    dma = pltpu.SemaphoreType.DMA
    scratch = [
        V((n, rows, width + 128), BF16),
        V((n, 32, width), BF16),
        V((n, block, 128), BF16),
        V((seqs, width), F32),
        V((seqs, width), BF16),
        V((width, ff), BF16),
        V((width, ff), BF16),
        V((ff, width), BF16),
        V((128, seqs), F32),
        V((128, seqs), F32),
        V((128, seqs), F32),
        V((128, seqs), F32),
        V((4 * slots, width), BF16),
        V((4, block, 128), BF16),
        V((4 * slots, ff), BF16),
        V((4, 64 + slots, width), BF16),
        V((2, chips, rows, width), BF16),
        V((chips, rows, width), BF16),
        V((2, hops, rows, width), BF16),
        V((2, hops, rows, width), BF16),
        V((seqs, 128), F32),
        V((128, width), BF16),
        V((128, width), BF16),
        V((seqs, 128), F32),
        V((seqs, 128), F32),
        V((2, 1, seqs), F32),
        V((n, 1, seqs // 2), F32),
        V((128, 128), F32),
        dma((17,)),
        dma((2,)),
    ]
    scratch += [dma((2, count)) for count in (4, 2, 4, 4, 8)]
    scratch += [dma((2, hops, 4))] * 2 + [dma((2,))] * 4 + [dma((2, hops + 1))] * 2
    scratch += [dma((4,)), dma((4,))] + [dma((1,))] * 4
    layer_out, new_re, new_im = pl.pallas_call(
        functools.partial(kernel, n, (rows, width, ff, cap)),
        out_shape=(
            jax.ShapeDtypeStruct((rows, width), BF16),
            jax.ShapeDtypeStruct((128, seqs), F32),
            jax.ShapeDtypeStruct((128, seqs), F32),
        ),
        in_specs=in_specs,
        out_specs=(vmem, far, far),
        scratch_shapes=scratch,
        compiler_params=pltpu.CompilerParams(
            collective_id=0, has_side_effects=True, vmem_limit_bytes=66_000_000
        ),
        name="layer_step",
    )(*operands)
    layer_out, new_re, new_im = pl.pallas_call(
        finish,
        out_shape=(
            jax.ShapeDtypeStruct((rows, width), BF16),
            jax.ShapeDtypeStruct((128, seqs), F32),
            jax.ShapeDtypeStruct((128, seqs), F32),
        ),
        in_specs=(far,) * 3,
        out_specs=(far,) * 3,
        scratch_shapes=[V((rows, width), BF16), V((128, seqs), F32), V((128, seqs), F32), dma((5,)), dma((5,))],
        name="write_out",
    )(layer_out, new_re, new_im)
    groups, state = state_real.shape[1:]

    def back(values):
        return values.reshape(groups, state, seqs).transpose(2, 0, 1)

    return (layer_out, back(new_re), back(new_im))


def solution(mesh):
    both = ("grp", "ep")
    return jax.shard_map(
        on_device,
        mesh=mesh,
        in_specs=(
            P(both, None),
            P(both, None),
            P(both, None),
            P("grp", "ep", None),
            P("grp", "ep", None),
            P(),
            P(None, "ep"),
            P("ep", None),
            P("ep", None),
            P("ep"),
            P("ep", None, None),
            P("ep", None, None),
            P("ep", None, None),
            P("ep", None, None),
            P("ep", None),
            P("ep", None),
            P(),
            P("ep", None, None),
            P("ep", None, None),
            P("ep", None, None),
            P(None, "ep"),
            P(None, "ep"),
            P("ep", None),
            P("ep"),
        ),
        out_specs=(P(both, None), P("grp", "ep", None), P("grp", "ep", None)),
        check_vma=False,
    )
```
